32 devices in a mesh: kv: 8 (over z, x), tp: 4 (over y, core).
Axes of the slice: x: 2, y: 2, z: 4, core: 2. Of those that a mesh axis runs over, the one named last changes fastest.
Arguments:
- stream: bfloat16 [128, 4096], P(None, ('kv', 'tp')), may hold values from -20 to 20
- ssm_state: float32 [128, 64, 64, 128], P('kv', 'tp'), may hold values from -1.8 to 1.8
- conv_state: bfloat16 [128, 3, 8, 768], P('kv', None, 'tp'), may hold values from -6 to 6
- first_gain: float32 [4096], P(('kv', 'tp')), may hold values from 0.1 to 1.9
- first_gate: bfloat16 [4096, 11264], P('kv', 'tp'), may hold values from -0.09375 to 0.09375
- first_up: bfloat16 [4096, 11264], P('kv', 'tp'), may hold values from -0.09375 to 0.09375
- first_down: bfloat16 [11264, 4096], P('tp', 'kv'), may hold values from -0.0546875 to 0.0546875
- mix_gain: float32 [4096], P(('kv', 'tp')), may hold values from 0.1 to 1.9
- gate_in: bfloat16 [4096, 4096], P('kv', 'tp'), may hold values from -0.09375 to 0.09375
- value_in: bfloat16 [4096, 4096], P('kv', 'tp'), may hold values from -0.09375 to 0.09375
- write_in: bfloat16 [4096, 1024], P('kv', 'tp'), may hold values from -0.09375 to 0.09375
- read_in: bfloat16 [4096, 1024], P('kv', 'tp'), may hold values from -0.09375 to 0.09375
- step_in: bfloat16 [4096, 64], P('kv', 'tp'), may hold values from -0.09375 to 0.09375
- conv_weight: float32 [4, 8, 768], P(None, 'tp'), may hold values from -3 to 3
- step_bias: float32 [64], P('tp'), may hold values from -3 to 0.5
- log_decay_rate: float32 [64], P('tp'), may hold values from -1 to 2.5
- group_gain: float32 [4096], P('tp'), may hold values from 0.1 to 1.9
- out_weight: bfloat16 [4096, 4096], P('tp', 'kv'), may hold values from -0.09375 to 0.09375
- last_norm_gain: float32 [4096], P(('kv', 'tp')), may hold values from 0.1 to 1.9
- second_gate: bfloat16 [4096, 11264], P('kv', 'tp'), may hold values from -0.09375 to 0.09375
- second_up: bfloat16 [4096, 11264], P('kv', 'tp'), may hold values from -0.09375 to 0.09375
- second_down: bfloat16 [11264, 4096], P('tp', 'kv'), may hold values from -0.109375 to 0.109375
Outputs:
- next_stream: bfloat16 [128, 4096], P(None, ('kv', 'tp'))
- ssm_next: float32 [128, 64, 64, 128], P('kv', 'tp')
- conv_next: bfloat16 [128, 3, 8, 768], P('kv', None, 'tp')
The draws below stay inside these ranges and needn't reach their ends.
All inputs are finite; a program needn't handle non-finite values.
Results may differ from the reference program's by a relative error of at most 0.015.
Values may be sent and summed in bfloat16 or wider, within the bound.
No kernel may reach another device: no remote copies, remote signals or barrier semaphores. Data moves between devices by JAX's collectives and lax.ppermute only.
A program may use at most 128 MiB of HBM per device.

```python
import jax
import jax.numpy as jnp
from jax import lax

D = 4096
FF = 11264
HEADS = 64
HEAD_DIM = 64
STATE = 128
GROUPS = 8
TAPS = 4
SEQS = 128
GROUP_CH = 768
N_KV = 8
N_TP = 4


def draw_stream(key, part):
    noise_key = jax.random.fold_in(jax.random.fold_in(key, 11), 0)
    shard_width = D // (N_KV * N_TP)
    column = jnp.arange(D, dtype=jnp.int32)
    tp_index = column // shard_width % N_TP
    kv_index = column // (shard_width * N_TP)
    tp_frac = tp_index.astype(jnp.float32) / max(N_TP - 1, 1)
    kv_frac = kv_index.astype(jnp.float32) / max(N_KV - 1, 1)
    column_scale = jnp.exp(jnp.log(0.3) + jnp.log(10.0) * tp_frac + jnp.log(1.3) * kv_frac)[None]
    base = jax.random.truncated_normal(noise_key, -4.0, 4.0, (SEQS, D), jnp.float32)
    return (base * column_scale).astype(jnp.bfloat16)


def level_of(rng, dims, cuts, least, high):
    def one(dim, blocks):
        steps = jax.random.uniform(jax.random.fold_in(jax.random.fold_in(rng, 6), dim), (blocks,), jnp.float32, least / len(cuts), high / len(cuts))
        return jnp.repeat(jnp.exp(steps), dims[dim] // blocks).reshape((-1,) + (1,) * (len(dims) - dim - 1))

    loudness = one(*cuts[0])
    for cut in cuts[1:]:
        loudness = loudness * one(*cut)
    return loudness


def scatter_about(key, dims, scale, limit, pieces=(), held_as=jnp.bfloat16):
    result = scale * jax.random.normal(key, dims, jnp.float32)
    if pieces:
        result = result * level_of(key, dims, pieces, -0.22, 0.18)
    return jnp.clip(result, -limit, limit).astype(held_as)


def setup_inputs(seed: int = 0) -> dict:
    seeds = jax.random.split(jax.random.key(seed), 23)
    stream = draw_stream(jax.random.fold_in(seeds[22], 71), 0)
    ssm_state = scatter_about(seeds[1], (SEQS, HEADS, HEAD_DIM, STATE), 0.3, 1.8, ((0, 8), (1, 4)), jnp.float32)
    conv_state = scatter_about(seeds[2], (SEQS, TAPS - 1, GROUPS, GROUP_CH), 1.0, 6.0, ((0, 8), (2, 4)))
    first_gain = jnp.clip(1.0 + 0.18 * jax.random.normal(seeds[3], (D,), jnp.float32), 0.1, 1.9)
    first_gate = scatter_about(seeds[4], (D, FF), D ** -0.5, 0.09375, ((0, 8), (1, 4)))
    first_up = scatter_about(seeds[5], (D, FF), D ** -0.5, 0.09375, ((0, 8), (1, 4)))
    first_down = scatter_about(seeds[6], (FF, D), FF ** -0.5, 0.0546875, ((0, 4), (1, 8)))
    mix_gain = jnp.clip(1.0 + 0.18 * jax.random.normal(seeds[7], (D,), jnp.float32), 0.1, 1.9)
    gate_in = scatter_about(seeds[8], (D, HEADS * HEAD_DIM), D ** -0.5, 0.09375, ((0, 8), (1, 4)))
    value_in = scatter_about(seeds[9], (D, HEADS * HEAD_DIM), D ** -0.5, 0.09375, ((0, 8), (1, 4)))
    write_in = scatter_about(seeds[10], (D, GROUPS * STATE), D ** -0.5, 0.09375, ((0, 8), (1, 4)))
    read_in = scatter_about(seeds[11], (D, GROUPS * STATE), D ** -0.5, 0.09375, ((0, 8), (1, 4)))
    step_in = scatter_about(seeds[12], (D, HEADS), D ** -0.5, 0.09375, ((0, 8), (1, 4)))
    conv_weight = scatter_about(seeds[13], (TAPS, GROUPS, GROUP_CH), TAPS ** -0.5, 3.0, ((1, 4),), jnp.float32)
    step_bias = jnp.clip(-3.0 + 3.5 * jax.random.uniform(seeds[14], (HEADS,), jnp.float32) ** level_of(seeds[14], (HEADS,), ((0, 4),), -0.2, 0.2), -3.0, 0.5)
    log_decay_rate = jnp.clip(-1.0 + 3.5 * jax.random.uniform(seeds[15], (HEADS,), jnp.float32) ** level_of(seeds[15], (HEADS,), ((0, 4),), -0.2, 0.2), -1.0, 2.5)
    group_gain = jnp.clip(1.0 + 0.18 * jax.random.normal(seeds[16], (HEADS * HEAD_DIM,), jnp.float32), 0.1, 1.9)
    out_weight = scatter_about(seeds[17], (HEADS * HEAD_DIM, D), (HEADS * HEAD_DIM) ** -0.5, 0.09375, ((0, 4), (1, 8)))
    last_norm_gain = jnp.clip(1.0 + 0.18 * jax.random.normal(seeds[18], (D,), jnp.float32), 0.1, 1.9)
    second_gate = scatter_about(seeds[19], (D, FF), D ** -0.5, 0.09375, ((0, 8), (1, 4)))
    second_up = scatter_about(seeds[20], (D, FF), D ** -0.5, 0.09375, ((0, 8), (1, 4)))
    second_down = scatter_about(seeds[21], (FF, D), (FF // 4) ** -0.5, 0.109375, ((0, 4), (1, 8)))
    return dict(stream=stream, ssm_state=ssm_state, conv_state=conv_state, first_gain=first_gain, first_gate=first_gate, first_up=first_up, first_down=first_down, mix_gain=mix_gain, gate_in=gate_in, value_in=value_in, write_in=write_in, read_in=read_in, step_in=step_in, conv_weight=conv_weight, step_bias=step_bias, log_decay_rate=log_decay_rate, group_gain=group_gain, out_weight=out_weight, last_norm_gain=last_norm_gain, second_gate=second_gate, second_up=second_up, second_down=second_down)


norm_epsilon = 1e-06

def norm_rows(stream, gain):
    values = stream.astype(jnp.float32)
    scaled = (values * gain.astype(jnp.float32)[None]).astype(jnp.bfloat16)
    factor = lax.rsqrt(lax.optimization_barrier(jnp.mean(values * values, axis=1, keepdims=True)) + norm_epsilon)
    return (scaled, factor)

def blockwise_down(hidden, weight_matrix):
    batch = hidden.shape[0]
    block_list = hidden.reshape(batch, N_TP, -1).astype(jnp.float32)
    split_pieces = weight_matrix.reshape(N_TP, -1, weight_matrix.shape[1]).astype(jnp.float32)
    value_partial_sum = jnp.einsum('noc,oci->noi', block_list, split_pieces).astype(jnp.bfloat16)
    value_partial_sum = lax.optimization_barrier(value_partial_sum)
    return lax.optimization_barrier(jnp.sum(value_partial_sum.astype(jnp.float32), axis=1))

def channel_mixer(stream, gain, gate_weight, up_weight, down_weight):
    scaled, factor = norm_rows(stream, gain)
    gate = jnp.dot(scaled, gate_weight, preferred_element_type=jnp.float32) * factor
    up_sum = jnp.dot(scaled, up_weight, preferred_element_type=jnp.float32) * factor
    hidden = (jax.nn.silu(gate) * up_sum).astype(jnp.bfloat16)
    branch_output = blockwise_down(hidden, down_weight)
    return (stream.astype(jnp.float32) + 0.5 * branch_output).astype(jnp.bfloat16)

def token_mixer(stream, ssm_state, conv_state, gain, gate_in, value_in, write_in, read_in, step_in, conv_weight, step_bias, log_decay_rate, group_gain, out_weight):
    scaled, factor = norm_rows(stream, gain)

    def project(weight_matrix):
        return (jnp.dot(scaled, weight_matrix, preferred_element_type=jnp.float32) * factor).astype(jnp.bfloat16)
    gate = project(gate_in)
    values = project(value_in)
    writes = project(write_in)
    reads = project(read_in)
    steps = project(step_in)
    batch = stream.shape[0]
    groups = conv_weight.shape[1]
    state_size = write_in.shape[1] // groups
    heads = step_in.shape[1]
    head_size = value_in.shape[1] // heads
    per_group = heads // groups
    width = per_group * head_size
    fresh = jnp.concatenate([values.reshape(batch, groups, width), writes.reshape(batch, groups, state_size), reads.reshape(batch, groups, state_size)], axis=2)
    window = jnp.concatenate([conv_state, fresh[:, None]], axis=1)
    activated = jax.nn.silu(lax.optimization_barrier(jnp.sum(window.astype(jnp.float32) * conv_weight.astype(jnp.float32)[None], axis=1)))
    inputs = activated[:, :, :width].reshape(batch, groups, per_group, head_size)
    write_vec = activated[:, :, width:width + state_size]
    read_vec = activated[:, :, width + state_size:]
    step_size = jax.nn.softplus(steps.astype(jnp.float32) + step_bias[None])
    decay = jnp.exp(-step_size * jnp.exp(log_decay_rate)[None])
    step_size = step_size.reshape(batch, groups, per_group)
    decay = decay.reshape(batch, groups, per_group)
    carried = ssm_state.reshape(batch, groups, per_group, head_size, state_size)
    updated = carried * decay[:, :, :, None, None] + (step_size[:, :, :, None] * inputs)[..., None] * write_vec[:, :, None, None, :]
    readout = jnp.einsum('bghpn,bgn->bghp', updated, read_vec).reshape(batch, groups, width)
    gated = readout * jax.nn.silu(gate.astype(jnp.float32)).reshape(batch, groups, width)
    normed = gated * lax.rsqrt(lax.optimization_barrier(jnp.mean(gated * gated, axis=2, keepdims=True)) + norm_epsilon)
    mixed = (normed * group_gain.reshape(groups, width)[None]).astype(jnp.bfloat16).reshape(batch, groups * width)
    branch_output = blockwise_down(mixed, out_weight)
    after = (stream.astype(jnp.float32) + branch_output).astype(jnp.bfloat16)
    return (after, updated.reshape(ssm_state.shape), window[:, 1:])

def reference(stream, ssm_state, conv_state, first_gain, first_gate, first_up, first_down, mix_gain, gate_in, value_in, write_in, read_in, step_in, conv_weight, step_bias, log_decay_rate, group_gain, out_weight, last_norm_gain, second_gate, second_up, second_down):
    after_first = channel_mixer(stream, first_gain, first_gate, first_up, first_down)
    after_mix, ssm_next, conv_next = token_mixer(after_first, ssm_state, conv_state, mix_gain, gate_in, value_in, write_in, read_in, step_in, conv_weight, step_bias, log_decay_rate, group_gain, out_weight)
    next_stream = channel_mixer(after_mix, last_norm_gain, second_gate, second_up, second_down)
    return (next_stream, ssm_next, conv_next)
```

```python
import functools

import jax
import jax.numpy as jnp
from jax import lax
from jax.experimental import pallas as pl
from jax.experimental.pallas import tpu as pltpu
from jax.sharding import PartitionSpec as P

norm_epsilon = 1e-06
LANES = 128
f32, bf16 = jnp.float32, jnp.bfloat16


VMEM = pl.BlockSpec(memory_space=pltpu.VMEM)
SMEM = pl.BlockSpec(memory_space=pltpu.SMEM)
ANY = pl.BlockSpec(memory_space=pl.ANY)


def call(kernel, name, ins, outs, scratch=(), flops=0, limit=16):
    moved = sum(a.size * a.dtype.itemsize for a, _ in ins)
    return pl.pallas_call(
        kernel,
        out_shape=[jax.ShapeDtypeStruct(s, d) for s, d in outs],
        in_specs=[s for _, s in ins],
        out_specs=[VMEM] * len(outs),
        scratch_shapes=list(scratch),
        compiler_params=pltpu.CompilerParams(vmem_limit_bytes=limit * 2**20),
        cost_estimate=pl.CostEstimate(flops=max(flops, 1000), bytes_accessed=moved, transcendentals=0),
        name=name,
    )(*[a for a, _ in ins])


class Grid:
    def __init__(self, rows):
        self.kv, self.tp = lax.axis_size("kv"), lax.axis_size("tp")
        self.I = 1
        while (self.I * 2) ** 2 <= self.kv:
            self.I *= 2
        self.O = self.kv // self.I
        self.rows = rows
        self.r = rows // self.kv
        self.offset = [s * self.I + t for t in range(self.I) for s in range(self.O)]

    def inner(self, x, t):
        return lax.ppermute(x, "kv", [(i, i ^ t) for i in range(self.kv)])

    def outer(self, x, s):
        return lax.ppermute(x, "kv", [(i, i ^ (s * self.I)) for i in range(self.kv)])

    def tpx(self, x, m):
        return lax.ppermute(x, "tp", [(i, i ^ m) for i in range(self.tp)])


def columns_at(ref, index, cols, count):
    if cols % LANES == 0:
        return ref[:, pl.ds(pl.multiple_of(index * cols, cols), cols)]
    block = ref[:, :cols]
    for c in range(1, count):
        block = jnp.where(index == c, ref[:, c * cols : (c + 1) * cols], block)
    return block


def prologue(grid, where, stream, gains):
    r, n = grid.r, grid.rows

    def kernel(where_ref, x_ref, a_ref, b_ref, c_ref, o_ref):
        k = where_ref[0]
        for j, m in enumerate(grid.offset):
            at = pl.multiple_of((k ^ m) * r, r)
            o_ref[j * r : (j + 1) * r, :] = x_ref[pl.ds(at, r), :]
        high, mid, low = [], [], []
        for ref in (a_ref, b_ref, c_ref):
            g = ref[...]
            h = g.astype(bf16).astype(f32)
            m = (g - h).astype(bf16).astype(f32)
            high.append(h)
            mid.append(m)
            low.append(g - h - m)
        pad = jnp.zeros((7, g.shape[1]), f32)
        o_ref[n : n + 16, :] = jnp.concatenate(high + mid + low + [pad], axis=0).astype(bf16)

    ins = [(where, SMEM), (stream, VMEM)] + [(g[None], VMEM) for g in gains]
    return call(kernel, "prologue", ins, [((n + 16, stream.shape[1]), bf16)])[0]


def scaled_and_squares(x, gain, scaled_ref, extra_ref):
    scaled_ref[...] = (x * gain).astype(bf16)
    sq = jnp.sum(x * x, axis=1, keepdims=True)
    high = sq.astype(bf16).astype(f32)
    lane = lax.broadcasted_iota(jnp.int32, extra_ref.shape, 1)
    both = jnp.where(lane == LANES - 2, high, jnp.where(lane == LANES - 1, sq - high, 0.0))
    extra_ref[...] = both.astype(bf16)


def first_norm(grid, gathered):
    n, width = grid.rows, gathered.shape[1]

    def kernel(g_ref, x_ref, scaled_ref, extra_ref, gains_ref):
        terms = g_ref[n : n + 16, :].astype(f32)
        gains = terms[0:3] + terms[3:6] + terms[6:9]
        gains_ref[...] = gains
        x = g_ref[0:n, :]
        x_ref[...] = x
        scaled_and_squares(x.astype(f32), gains[0:1], scaled_ref, extra_ref)

    outs = [((n, width), bf16), ((n, width), bf16), ((n, LANES), bf16), ((3, width), f32)]
    return call(kernel, "first_norm", [(gathered, VMEM)], outs)


def residual_norm(grid, gathered, x, gains, index, weight):
    n, width = x.shape

    def kernel(g_ref, x_ref, gain_ref, after_ref, scaled_ref, extra_ref):
        total = g_ref[0:n, :].astype(f32)
        for m in range(1, grid.tp):
            total += g_ref[m * n : (m + 1) * n, :].astype(f32)
        after = (x_ref[...].astype(f32) + weight * total).astype(bf16)
        after_ref[...] = after
        scaled_and_squares(after.astype(f32), gain_ref[index : index + 1, :], scaled_ref, extra_ref)

    outs = [((n, width), bf16), ((n, width), bf16), ((n, LANES), bf16)]
    return call(kernel, "residual_norm", [(gathered, VMEM), (x, VMEM), (gains, VMEM)], outs)


def store_rows(grid, inner_first, outs, value, at):
    r, I, O = grid.r, grid.I, grid.O
    width = value.shape[1]
    value = value.astype(bf16)
    if inner_first:
        for t in range(I):
            outs[t][:, at : at + width] = value[t * O * r : (t + 1) * O * r]
    else:
        for s in range(O):
            for t in range(I):
                j = (t * O + s) * r
                outs[s][t * r : (t + 1) * r, at : at + width] = value[j : j + r]


def part_shapes(grid, inner_first, width):
    n = grid.I if inner_first else grid.O
    return [((grid.rows // n, width), bf16)] * n


def ff_project(grid, scaled, extra, gate, up, first, count, inner_first):
    depth = gate.shape[0]
    tile = next(t for t in (512, 384, 256, 128) if count % t == 0)
    steps = count // tile
    width = 2 * count + (0 if inner_first else LANES)
    shapes = part_shapes(grid, inner_first, width)

    def kernel(x_ref, e_ref, g_hbm, u_hbm, *rest):
        outs, (g_buf, u_buf, sems) = rest[: len(shapes)], rest[len(shapes) :]
        copies = []
        for j in range(steps):
            for i, (src, buf) in enumerate(((g_hbm, g_buf), (u_hbm, u_buf))):
                here = pl.ds(j * tile, tile)
                c = pltpu.make_async_copy(
                    src.at[:, pl.ds(first + j * tile, tile)], buf.at[:, here], sems.at[i, j]
                )
                c.start()
                copies.append((c, buf, i * count + j * tile, j * tile))
        x = x_ref[...]
        if not inner_first:
            store_rows(grid, inner_first, outs, e_ref[...], 2 * count)
        for c, buf, at, src in copies:
            c.wait()
            value = jnp.dot(x, buf[:, src : src + tile], preferred_element_type=f32)
            store_rows(grid, inner_first, outs, value, at)

    scratch = [pltpu.VMEM((depth, count), bf16)] * 2 + [pltpu.SemaphoreType.DMA((2, steps))]
    ins = [(scaled, VMEM), (extra, VMEM), (gate, ANY), (up, ANY)]
    return call(kernel, "ff_project", ins, shapes, scratch, flops=4 * grid.rows * depth * count)


def add_split(grid, parts):
    r = grid.r
    n = parts[0].shape[0] // r
    width = parts[0].shape[1]

    def kernel(*refs):
        ins, outs = refs[: len(parts)], refs[len(parts) :]
        for b in list(range(1, n)) + [0]:
            total = ins[0][b * r : (b + 1) * r, :].astype(f32)
            for ref in ins[1:]:
                total += ref[b * r : (b + 1) * r, :].astype(f32)
            outs[b][...] = total.astype(outs[b].dtype)

    outs = [((r, width), f32 if b == 0 else bf16) for b in range(n)]
    return call(kernel, "add_split", [(p, VMEM) for p in parts], outs)


def scatter_rows(grid, parts, inner_first):
    I, O = grid.I, grid.O
    first, second = (grid.inner, grid.outer) if inner_first else (grid.outer, grid.inner)
    n_first, n_second = (I, O) if inner_first else (O, I)
    got = [first(parts[t], t) for t in range(1, n_first)]
    pieces = add_split(grid, [parts[0]] + got)
    return [pieces[0]] + [second(pieces[s], s) for s in range(1, n_second)]


def total_of(refs):
    total = refs[0][...]
    for ref in refs[1:]:
        total += ref[...].astype(f32)
    return total


def factor_of(block, width):
    squares = block[:, LANES - 2 : LANES - 1] + block[:, LANES - 1 : LANES]
    return lax.rsqrt(squares / width + norm_epsilon)


def ff_hidden(grid, terms, factor, width):
    last = factor is None
    r = terms[0].shape[0]
    count = (terms[0].shape[1] - (LANES if last else 0)) // 2

    def kernel(*refs):
        ins, outs = refs[: len(terms)], refs[len(terms) :]
        total = total_of(ins)
        if last:
            factor = factor_of(total[:, 2 * count :], width)
            outs[1][...] = jnp.broadcast_to(factor, outs[1].shape)
        else:
            factor = outs[0][:, 0:1]
            outs = outs[1:]
        gate = total[:, :count] * factor
        hidden = gate / (1.0 + jnp.exp(-gate)) * (total[:, count : 2 * count] * factor)
        outs[0][...] = hidden.astype(bf16)

    ins = [(t, VMEM) for t in terms] + ([] if last else [(factor, VMEM)])
    outs = [((r, count), bf16)] + ([((r, LANES), f32)] if last else [])
    return call(kernel, "ff_hidden", ins, outs)


def gather_rows(grid, x, inner_first):
    I, O = grid.I, grid.O
    if inner_first:
        pair = jnp.concatenate([x] + [grid.inner(x, t) for t in range(1, I)], axis=0)
        arrays = [pair] + [grid.outer(pair, s) for s in range(1, O)]
        blocks = [[t * O + s for t in range(I)] for s in range(O)]
    else:
        group = jnp.concatenate([x] + [grid.outer(x, s) for s in range(1, O)], axis=0)
        arrays = [group] + [grid.inner(group, t) for t in range(1, I)]
        blocks = [[t * O + s for s in range(O)] for t in range(I)]
    return list(zip(arrays, blocks))


def down_project(grid, sides, weight, split, where):
    depth, width = weight.shape
    r, n = grid.r, grid.rows
    arrays = [(a, VMEM) for side in sides for a, _ in side]
    counts = [side[0][0].shape[1] for side in sides]
    edges = [sum(counts[:i]) for i in range(len(counts) + 1)]
    tp, cols = grid.tp, width // grid.tp
    if split:
        outs = [((n, cols * (tp // 2)), bf16), ((n, cols * (tp // 2 - 1)), f32), ((n, cols), f32)]
    else:
        outs = [((n, width), bf16)]

    def kernel(where_ref, *refs):
        ins, refs = refs[: len(arrays)], refs[len(arrays) :]
        w_hbm, refs = refs[0], refs[1:]
        out_refs, (w_buf, acc, sems) = refs[: len(outs)], refs[len(outs) :]
        copies = []
        for i, count in enumerate(counts):
            rows = pl.ds(edges[i], count)
            c = pltpu.make_async_copy(w_hbm.at[rows, :], w_buf.at[rows, :], sems.at[i])
            c.start()
            copies.append(c)
        at, total = 0, None
        for i, side in enumerate(sides):
            pieces = [None] * grid.kv
            for _, blocks in side:
                for p, b in enumerate(blocks):
                    pieces[b] = ins[at][p * r : (p + 1) * r, :]
                at += 1
            lhs = jnp.concatenate(pieces, axis=0)
            copies[i].wait()
            product = jnp.dot(lhs, w_buf[edges[i] : edges[i + 1], :], preferred_element_type=f32)
            total = product if total is None else total + product
        if not split:
            out_refs[0][...] = total.astype(bf16)
            return
        acc[...] = total
        me = where_ref[1]
        for m in range(tp):
            block = columns_at(acc, me ^ m, cols, tp)
            h = m // 2
            if m % 2:
                out_refs[0][:, h * cols : (h + 1) * cols] = block.astype(bf16)
            elif h:
                out_refs[1][:, (h - 1) * cols : h * cols] = block
            else:
                out_refs[2][...] = block

    scratch = [
        pltpu.VMEM((depth, width), bf16),
        pltpu.VMEM((n, width) if split else (8, LANES), f32),
        pltpu.SemaphoreType.DMA((len(sides),)),
    ]
    ins = [(where, SMEM)] + arrays + [(weight, ANY)]
    return call(kernel, "down_project", ins, outs, scratch, flops=2 * n * depth * width)


def finish(grid, where, parts, x, weight):
    for_partner, others, own = parts
    n, cols = own.shape
    r, more = grid.r, grid.tp // 2 - 1
    got = grid.tpx(for_partner, 1)

    def middle(g_ref, o_ref, own_ref, own_out, *outs):
        own_out[...] = own_ref[...] + g_ref[:, :cols].astype(f32)
        for h in range(more):
            here = slice(h * cols, (h + 1) * cols)
            there = slice((h + 1) * cols, (h + 2) * cols)
            outs[h][...] = (o_ref[:, here] + g_ref[:, there].astype(f32)).astype(bf16)

    shapes = [((n, cols), f32)] + [((n, cols), bf16)] * more
    ins = [(got, VMEM), (others, VMEM), (own, VMEM)]
    sums = call(middle, "finish_middle", ins, shapes)
    arrived = [grid.tpx(sums[h], 2 * h) for h in range(1, more + 1)]

    def kernel(where_ref, x_ref, *refs):
        ins, o_ref = refs[:-1], refs[-1]
        total = total_of(ins)
        mine = columns_at(x_ref, where_ref[1], cols, grid.tp).astype(f32)
        after = (mine + weight * total).astype(bf16)
        k = where_ref[0]
        for j, m in enumerate(grid.offset):
            o_ref[pl.ds(pl.multiple_of((k ^ m) * r, r), r), :] = after[j * r : (j + 1) * r]

    ins = [(where, SMEM), (x, VMEM), (sums[0], VMEM)] + [(a, VMEM) for a in arrived]
    return call(kernel, "finish", ins, [((n, cols), bf16)])[0]


def channel_mixer(grid, scaled, extra, gate, up, down, width, where, split):
    blocks = gate.shape[1] // LANES
    count = blocks * 2 // 3 * LANES
    rest = gate.shape[1] - count
    outer_parts = ff_project(grid, scaled, extra, gate, up, count, rest, False)
    inner_parts = ff_project(grid, scaled, extra, gate, up, 0, count, True)
    outer_terms = scatter_rows(grid, outer_parts, False)
    inner_terms = scatter_rows(grid, inner_parts, True)
    hidden_b, factor = ff_hidden(grid, outer_terms, None, width)
    (hidden_a,) = ff_hidden(grid, inner_terms, factor, width)
    sides = [gather_rows(grid, hidden_a, False), gather_rows(grid, hidden_b, True)]
    return down_project(grid, sides, down, split, where)


def mix_project(grid, scaled, extra, gate_in, value_in, write_in, read_in, step_in, groups):
    depth = gate_in.shape[0]
    per, state = value_in.shape[1] // groups, write_in.shape[1] // groups
    channels = per + 2 * state
    width = groups * channels + LANES
    heads = step_in.shape[1]
    shapes_a = part_shapes(grid, True, width)
    shapes_b = part_shapes(grid, False, gate_in.shape[1])

    def kernel(x_ref, e_ref, s_ref, g_hbm, v_hbm, w_hbm, r_hbm, *rest):
        outs_a, rest = rest[: len(shapes_a)], rest[len(shapes_a) :]
        outs_b, rest = rest[: len(shapes_b)], rest[len(shapes_b) :]
        bufs, sems = rest[:4], rest[4]
        copies = []
        for i, (src, buf) in enumerate(zip((g_hbm, v_hbm, w_hbm, r_hbm), bufs)):
            c = pltpu.make_async_copy(src, buf, sems.at[i])
            c.start()
            copies.append(c)
        x = x_ref[...]
        e = e_ref[...].astype(f32)
        copies[0].wait()
        value = jnp.dot(x, bufs[0][...], preferred_element_type=f32)
        store_rows(grid, False, outs_b, value, 0)
        steps = jnp.dot(x, s_ref[...], preferred_element_type=f32)
        steps = jnp.concatenate([steps, e[:, heads:]], axis=1)
        store_rows(grid, True, outs_a, steps, groups * channels)
        for i, (size, at) in enumerate(((per, 0), (state, per), (state, per + state)), 1):
            copies[i].wait()
            for g in range(groups):
                value = jnp.dot(x, bufs[i][:, g * size : (g + 1) * size], preferred_element_type=f32)
                store_rows(grid, True, outs_a, value, g * channels + at)

    weights = [gate_in, value_in, write_in, read_in]
    scratch = [pltpu.VMEM(w.shape, bf16) for w in weights] + [pltpu.SemaphoreType.DMA((4,))]
    ins = [(scaled, VMEM), (extra, VMEM), (step_in, VMEM)] + [(w, ANY) for w in weights]
    flops = 2 * grid.rows * depth * (width + gate_in.shape[1])
    parts = call(kernel, "mix_project", ins, shapes_a + shapes_b, scratch, flops=flops)
    return parts[: len(shapes_a)], parts[len(shapes_a) :]


def mix_front(terms, convolved, last_tap, step_bias, log_decay_rate, width):
    r, channels = convolved.shape
    heads = step_bias.shape[0]

    def kernel(*refs):
        ins, refs = refs[: len(terms)], refs[len(terms) :]
        conv_ref, tap_ref, bias_ref, rate_ref = refs[:4]
        fresh_ref, act_ref, step_ref, decay_ref, factor_ref = refs[4:]
        total = total_of(ins)
        factor = factor_of(total[:, channels:], width)
        factor_ref[...] = jnp.broadcast_to(factor, factor_ref.shape)
        fresh = (total[:, :channels] * factor).astype(bf16)
        fresh_ref[...] = fresh
        mixed = conv_ref[...] + fresh.astype(f32) * tap_ref[...]
        act_ref[...] = mixed / (1.0 + jnp.exp(-mixed))
        raw = (total[:, channels : channels + heads] * factor).astype(bf16).astype(f32) + bias_ref[...]
        step = jnp.maximum(raw, 0.0) + jnp.log1p(jnp.exp(-jnp.abs(raw)))
        step_ref[...] = step
        decay_ref[...] = jnp.exp(-step * jnp.exp(rate_ref[...]))

    ins = [(t, VMEM) for t in terms]
    ins += [(convolved, VMEM), (last_tap[None], VMEM), (step_bias[None], VMEM), (log_decay_rate[None], VMEM)]
    outs = [((r, channels), bf16), ((r, channels), f32), ((r, heads), f32), ((r, heads), f32), ((r, LANES), f32)]
    return call(kernel, "mix_front", ins, outs)


def on_device(
    stream,
    ssm_state,
    conv_state,
    first_gain,
    first_gate,
    first_up,
    first_down,
    mix_gain,
    gate_in,
    value_in,
    write_in,
    read_in,
    step_in,
    conv_weight,
    step_bias,
    log_decay_rate,
    group_gain,
    out_weight,
    last_norm_gain,
    second_gate,
    second_up,
    second_down,
):
    grid = Grid(stream.shape[0])
    r = grid.r
    width_all = stream.shape[1] * grid.kv * grid.tp
    where = jnp.stack([lax.axis_index("kv"), lax.axis_index("tp")]).astype(jnp.int32)

    packed = prologue(grid, where, stream, (first_gain, mix_gain, last_norm_gain))
    gathered = lax.all_gather(packed, "tp", axis=1, tiled=True)
    x, scaled, extra, gains = first_norm(grid, gathered)

    (partial,) = channel_mixer(grid, scaled, extra, first_gate, first_up, first_down, width_all, where, False)
    gathered = lax.all_gather(partial, "tp", axis=0, tiled=True)
    after_first, scaled, extra = residual_norm(grid, gathered, x, gains, 1, 0.5)

    taps, groups, group_ch = conv_weight.shape
    heads = step_in.shape[1]
    state_size = ssm_state.shape[3]
    head_size = ssm_state.shape[2]
    per_group = heads // groups
    width = per_group * head_size
    channels = groups * group_ch
    convolved = jnp.sum(conv_state.astype(f32) * conv_weight[None, : taps - 1], axis=1).reshape(r, channels)

    parts_a, parts_b = mix_project(
        grid, scaled, extra, gate_in, value_in, write_in, read_in, step_in, groups
    )
    terms_b = scatter_rows(grid, parts_b, False)
    terms_a = scatter_rows(grid, parts_a, True)
    fresh, activated, step_size, decay, factor = mix_front(
        terms_a, convolved, conv_weight[taps - 1].reshape(channels), step_bias, log_decay_rate, width_all
    )
    gate = terms_b[0]
    for term in terms_b[1:]:
        gate = gate + term.astype(f32)
    gate = (gate * factor[:, :1]).astype(bf16).astype(f32)

    carried = ssm_state.reshape(r, groups, per_group, head_size, state_size)

    def views(activated, step_size, decay):
        act = activated.reshape(r, groups, group_ch)
        inputs = act[:, :, :width].reshape(r, groups, per_group, head_size)
        return (
            inputs * step_size.reshape(r, groups, per_group, 1),
            act[:, :, width : width + state_size],
            act[:, :, width + state_size :],
            decay.reshape(r, groups, per_group, 1),
        )

    driven, write_vec, read_vec, kept = views(activated, step_size, decay)
    overlap = jnp.sum(write_vec * read_vec, axis=2)[:, :, None, None]
    readout = jnp.sum(carried * read_vec[:, :, None, None, :], axis=4) * kept + driven * overlap
    gated = readout.reshape(r, groups, width) * jax.nn.silu(gate).reshape(r, groups, width)
    normed = gated * lax.rsqrt(jnp.mean(gated * gated, axis=2, keepdims=True) + norm_epsilon)
    mixed = (normed * group_gain.reshape(groups, width)[None]).astype(bf16).reshape(r, groups * width)

    activated, step_size, decay, _ = lax.optimization_barrier((activated, step_size, decay, mixed))
    driven, write_vec, _, kept = views(activated, step_size, decay)
    ssm_next = carried * kept[..., None] + driven[..., None] * write_vec[:, :, None, None, :]
    ssm_next = ssm_next.reshape(ssm_state.shape)
    conv_next = jnp.concatenate([conv_state[:, 1:], fresh.reshape(r, 1, groups, group_ch)], axis=1)

    sides = [gather_rows(grid, mixed, False)]
    (partial,) = down_project(grid, sides, out_weight, False, where)
    gathered = lax.all_gather(partial, "tp", axis=0, tiled=True)
    after_mix, scaled, extra = residual_norm(grid, gathered, after_first, gains, 2, 1.0)

    parts = channel_mixer(grid, scaled, extra, second_gate, second_up, second_down, width_all, where, True)
    next_stream = finish(grid, where, parts, after_mix, 0.5)
    return (next_stream, ssm_next, conv_next)


def solution(mesh):
    return jax.shard_map(
        on_device,
        mesh=mesh,
        in_specs=(
            P(None, ("kv", "tp")),
            P("kv", "tp", None, None),
            P("kv", None, "tp", None),
            P(("kv", "tp")),
            P("kv", "tp"),
            P("kv", "tp"),
            P("tp", "kv"),
            P(("kv", "tp")),
            P("kv", "tp"),
            P("kv", "tp"),
            P("kv", "tp"),
            P("kv", "tp"),
            P("kv", "tp"),
            P(None, "tp", None),
            P("tp"),
            P("tp"),
            P("tp"),
            P("tp", "kv"),
            P(("kv", "tp")),
            P("kv", "tp"),
            P("kv", "tp"),
            P("tp", "kv"),
        ),
        out_specs=(P(None, ("kv", "tp")), P("kv", "tp", None, None), P("kv", None, "tp", None)),
        check_vma=False,
    )
```
